256 devices in a mesh: grp: 2 (over y), sp: 32 (over z, core), tp: 4 (over x).
Axes of the slice: x: 4, y: 2, z: 16, core: 2. Of those that a mesh axis runs over, the one named last changes fastest.
The devices are a block of a 4x16x16 slice.
Arguments:
- residual: bfloat16 [40960, 2048], P(('grp', 'sp', 'tp')), parts along dimension 0, may hold values from -40 to 40
- query_wide: bfloat16 [40960, 512], P(('grp', 'sp'), 'tp'), parts along dimension 0, may hold values from -6 to 6
- key_wide: bfloat16 [40960, 512], P(('grp', 'sp'), 'tp'), parts along dimension 0, may hold values from -6 to 6
- value_wide: bfloat16 [40960, 512], P(('grp', 'sp'), 'tp'), parts along dimension 0, may hold values from -6 to 6
- gate_wide: bfloat16 [40960, 512], P(('grp', 'sp'), 'tp'), parts along dimension 0, may hold values from -6 to 6
- write_wide: float32 [2, 4, 40960], P(None, 'tp', ('grp', 'sp')), parts along dimension 2, may hold values from -6 to 260
- keep_wide: float32 [2, 4, 40960], P(None, 'tp', ('grp', 'sp')), parts along dimension 2, may hold values from -1 to 18
- scale_wide: float32 [512], P('tp'), may hold values from 0.1 to 1.9
- query_narrow: bfloat16 [40960, 512], P(('grp', 'sp'), 'tp'), parts along dimension 0, may hold values from -6 to 6
- key_narrow: bfloat16 [40960, 512], P(('grp', 'sp'), 'tp'), parts along dimension 0, may hold values from -6 to 6
- value_narrow: bfloat16 [40960, 512], P(('grp', 'sp'), 'tp'), parts along dimension 0, may hold values from -6 to 6
- gate_narrow: bfloat16 [40960, 512], P(('grp', 'sp'), 'tp'), parts along dimension 0, may hold values from -6 to 6
- write_narrow: float32 [2, 8, 40960], P(None, 'tp', ('grp', 'sp')), parts along dimension 2, may hold values from -6 to 260
- keep_narrow: float32 [2, 8, 40960], P(None, 'tp', ('grp', 'sp')), parts along dimension 2, may hold values from -1 to 18
- scale_narrow: float32 [512], P('tp'), may hold values from 0.1 to 1.9
- output_wide: bfloat16 [512, 2048], P('tp'), may hold values from -0.1875 to 0.1875
- output_narrow: bfloat16 [512, 2048], P('tp'), may hold values from -0.1875 to 0.1875
- mixer_gain: float32 [2048], replicated, may hold values from 0.1 to 1.9
- up_weight: bfloat16 [2048, 8192], P('sp', 'tp'), may hold values from -0.125 to 0.125
- down_weight: bfloat16 [8192, 2048], P('tp', 'sp'), may hold values from -0.0625 to 0.0625
Outputs:
- result: bfloat16 [40960, 2048], P(('grp', 'sp', 'tp')), parts along dimension 0
The draws below stay inside these ranges and needn't reach their ends.
There are 2 independent parts, one for each index of `grp`. The reference program is written for one: setup_inputs(seed, part) draws one part's arguments, and reference() takes and returns one part's arrays. A program takes and returns all parts, laid end to end along the dimension named above; an argument that names none is the same for every part. Nothing has to cross between parts.
All inputs are finite; a program needn't handle non-finite values.
Results may differ from the reference program's by a relative error of at most 0.012.
Values may be sent and summed in bfloat16 or wider, within the bound.
A program may use at most 128 MiB of HBM per device.

```python
import math
import jax
import jax.numpy as jnp
from jax import lax

D = 2048
FF = 8192
HW = 4
DW = 128
HN = 8
DN = 64
BLOCK = 128
TOK_DEV = 640
SEQUENCE_TOKENS = 20480


def write_draw(key, count_of_heads):
    random_subkeys = jax.random.split(key, 1)
    return jnp.clip(jax.random.normal(random_subkeys[0], (2, count_of_heads, SEQUENCE_TOKENS), jnp.float32), -6.0, 6.0)


def keep_draw(key, count_of_heads):
    random_subkeys = jax.random.split(key, 5)
    ranking = jax.random.permutation(random_subkeys[0], count_of_heads)
    fast_heads = ranking < count_of_heads // 2
    log_rate = jnp.where(fast_heads, math.log(1.0 / 40.0), math.log(0.5 / SEQUENCE_TOKENS))[None, :, None]
    spread = jax.random.uniform(random_subkeys[1], (2, count_of_heads, SEQUENCE_TOKENS // TOK_DEV), jnp.float32, math.log(0.5), math.log(2.0))
    factor = jnp.repeat(spread, TOK_DEV, axis=2)
    jitter = 0.7 * jax.random.normal(random_subkeys[2], (2, count_of_heads, SEQUENCE_TOKENS), jnp.float32)
    sampled_values = -(log_rate + factor) + jitter
    spike_locations = jax.random.randint(random_subkeys[3], (2, count_of_heads, 3), 0, SEQUENCE_TOKENS)
    loss_terms = jax.random.uniform(random_subkeys[4], (2, count_of_heads, 3), jnp.float32, 0.5, 0.8)
    spike_magnitudes = jnp.log(loss_terms / (1.0 - loss_terms))
    spike_matches = jnp.arange(SEQUENCE_TOKENS)[None, None, None, :] == spike_locations[..., None]
    spike_gate = jnp.sum(jnp.where(spike_matches, spike_magnitudes[..., None], 0.0), axis=2)
    sampled_values = jnp.where(jnp.any(spike_matches, axis=2), spike_gate, sampled_values)
    return jnp.clip(sampled_values, -1.0, 18.0)


def draw_residual(key, part):
    random_subkeys = jax.random.split(key, 3)
    row_scale = jnp.exp(jax.random.uniform(random_subkeys[0], (SEQUENCE_TOKENS, 1), jnp.float32, math.log(0.4), math.log(2.5)))
    column_scale = jnp.exp(jax.random.uniform(random_subkeys[1], (1, D), jnp.float32, math.log(0.4), math.log(2.5)))
    sampled_values = jax.random.normal(random_subkeys[2], (SEQUENCE_TOKENS, D), jnp.float32) * row_scale * column_scale
    return jnp.clip(sampled_values, -40.0, 40.0).astype(jnp.bfloat16)


def draw_write_wide(key, part):
    return write_draw(key, HW)


def draw_write_narrow(key, part):
    return write_draw(key, HN)


def draw_keep_wide(key, part):
    return keep_draw(key, HW)


def draw_keep_narrow(key, part):
    return keep_draw(key, HN)


def level_of(stream_key, extent, pieces, least, high):
    gain, own = 1.0, jax.random.fold_in(stream_key, 6)
    for position, blocks in pieces:
        heights = jnp.exp(jax.random.uniform(jax.random.fold_in(own, position), (blocks,), jnp.float32, least / len(pieces), high / len(pieces)))
        gain = gain * jnp.repeat(heights, extent[position] // blocks).reshape([-1 if axis == position else 1 for axis in range(len(extent))])
    return gain


def scatter_about(key, dims, width, reach, shards=(), held_as=jnp.bfloat16):
    gain = level_of(key, dims, shards, -0.22, 0.18) if shards else 1.0
    result = jax.random.normal(key, dims, jnp.float32) * width * gain
    return jnp.minimum(jnp.maximum(result, -reach), reach).astype(held_as)


def setup_inputs(seed: int = 0, part: int = 0) -> dict:
    key_list = jax.random.split(jax.random.key(seed), 21)
    part_splits = jax.random.split(jax.random.fold_in(key_list[20], part), 21)
    return {
        "residual": draw_residual(jax.random.fold_in(jax.random.fold_in(key_list[20], part), 71), part),
        "query_wide": scatter_about(part_splits[1], (SEQUENCE_TOKENS, HW * DW), 1.0, 6.0, ((0, 32), (1, 4))),
        "key_wide": scatter_about(part_splits[2], (SEQUENCE_TOKENS, HW * DW), 1.0, 6.0, ((0, 32), (1, 4))),
        "value_wide": scatter_about(part_splits[3], (SEQUENCE_TOKENS, HW * DW), 1.0, 6.0, ((0, 32), (1, 4))),
        "gate_wide": scatter_about(part_splits[4], (SEQUENCE_TOKENS, HW * DW), 1.5, 6.0, ((0, 32), (1, 4))),
        "write_wide": draw_write_wide(jax.random.fold_in(jax.random.fold_in(key_list[20], part), 71), part),
        "keep_wide": draw_keep_wide(jax.random.fold_in(jax.random.fold_in(key_list[20], part), 71), part),
        "scale_wide": jnp.clip(1.0 + 0.18 * jax.random.normal(key_list[7], (HW * DW,), jnp.float32), 0.1, 1.9),
        "query_narrow": scatter_about(part_splits[8], (SEQUENCE_TOKENS, HN * DN), 1.0, 6.0, ((0, 32), (1, 4))),
        "key_narrow": scatter_about(part_splits[9], (SEQUENCE_TOKENS, HN * DN), 1.0, 6.0, ((0, 32), (1, 4))),
        "value_narrow": scatter_about(part_splits[10], (SEQUENCE_TOKENS, HN * DN), 1.0, 6.0, ((0, 32), (1, 4))),
        "gate_narrow": scatter_about(part_splits[11], (SEQUENCE_TOKENS, HN * DN), 1.5, 6.0, ((0, 32), (1, 4))),
        "write_narrow": draw_write_narrow(jax.random.fold_in(jax.random.fold_in(key_list[20], part), 71), part),
        "keep_narrow": draw_keep_narrow(jax.random.fold_in(jax.random.fold_in(key_list[20], part), 71), part),
        "scale_narrow": jnp.clip(1.0 + 0.18 * jax.random.normal(key_list[14], (HN * DN,), jnp.float32), 0.1, 1.9),
        "output_wide": scatter_about(key_list[15], (HW * DW, D), (HW * DW + HN * DN) ** -0.5, 0.1875, ((0, 4),)),
        "output_narrow": scatter_about(key_list[16], (HN * DN, D), (HW * DW + HN * DN) ** -0.5, 0.1875, ((0, 4),)),
        "mixer_gain": jnp.clip(1.0 + 0.18 * jax.random.normal(key_list[17], (D,), jnp.float32), 0.1, 1.9),
        "up_weight": scatter_about(key_list[18], (D, FF), D ** -0.5, 0.125, ((0, 32), (1, 4))),
        "down_weight": scatter_about(key_list[19], (FF, D), FF ** -0.5, 0.0625, ((0, 4), (1, 32))),
    }


START_LEVEL = -1e+30
EPSILON = 1e-06
HIGHEST_PRECISION = lax.Precision.HIGHEST

def to_heads(flat, count_of_heads):
    return flat.astype(jnp.float32).reshape(flat.shape[0], count_of_heads, -1).transpose(1, 0, 2)

def combine(earlier, later):
    ceiling = jnp.maximum(later[3] + earlier[2], later[2])
    former = jnp.exp(later[3] + earlier[2] - ceiling)
    latter = jnp.exp(later[2] - ceiling)
    memory = former[..., None, None] * earlier[0] + latter[..., None, None] * later[0]
    normal = former[..., None] * earlier[1] + latter[..., None] * later[1]
    return (memory, normal, ceiling, earlier[3] + later[3])

def prepare(query_heads, key_heads, value_heads, write_rows, log_keep):
    count_of_heads, length, head_size = query_heads.shape
    blocks = length // BLOCK
    block_shape = (count_of_heads, blocks, BLOCK, head_size)
    scaled = (query_heads * head_size ** (-0.5)).reshape(block_shape)
    key_blocks = key_heads.reshape(block_shape)
    value_blocks = value_heads.reshape(block_shape)
    write_blocks = write_rows.reshape(count_of_heads, blocks, BLOCK)
    cumulative = jnp.cumsum(log_keep.reshape(count_of_heads, blocks, BLOCK), axis=-1)
    totals = cumulative[..., -1]
    weight_log = totals[..., None] - cumulative + write_blocks
    local_peak = lax.optimization_barrier(jnp.max(weight_log, axis=-1))
    weights = jnp.exp(weight_log - local_peak[..., None])
    weighted = key_blocks * weights[..., None]
    memory = jnp.einsum('hnld,hnle->hnde', weighted, value_blocks, precision=HIGHEST_PRECISION)
    normal = lax.optimization_barrier(jnp.sum(weighted, axis=2))
    return ((scaled, key_blocks, value_blocks, write_blocks, cumulative), (memory, normal, local_peak, totals))

def block_starts(summary, start_state):

    def advance(carry, inputs):
        return (combine(carry, inputs), carry)
    stacked = tuple((jnp.moveaxis(member, 1, 0) for member in summary))
    final_state, starts = lax.scan(advance, start_state, stacked)
    return (final_state, tuple((jnp.moveaxis(member, 0, 1) for member in starts)))

def block_outputs(blocks_in, starts):
    scaled, key_blocks, value_blocks, write_blocks, cumulative = blocks_in
    memory, normal, carried_peak = (starts[0], starts[1], starts[2])
    positions = jnp.arange(BLOCK)
    causal = positions[:, None] >= positions[None, :]
    inner_log = jnp.where(causal, cumulative[..., :, None] - cumulative[..., None, :] + write_blocks[..., None, :], -jnp.inf)
    outer_log = cumulative + carried_peak[..., None]
    ceiling = jnp.maximum(lax.optimization_barrier(jnp.max(inner_log, axis=-1)), outer_log)
    inner_weight = jnp.exp(inner_log - ceiling[..., None])
    outer_weight = jnp.exp(outer_log - ceiling)
    scores = jnp.einsum('hnld,hnsd->hnls', scaled, key_blocks, precision=HIGHEST_PRECISION) * inner_weight
    numerator = jnp.einsum('hnls,hnse->hnle', scores, value_blocks, precision=HIGHEST_PRECISION) + outer_weight[..., None] * jnp.einsum('hnld,hnde->hnle', scaled, memory, precision=HIGHEST_PRECISION)
    denominator = lax.optimization_barrier(jnp.sum(scores, axis=-1)) + outer_weight * jnp.einsum('hnld,hnd->hnl', scaled, normal, precision=HIGHEST_PRECISION)
    outcome = numerator / jnp.maximum(jnp.abs(denominator), jnp.exp(-ceiling))[..., None]
    count_of_heads, blocks = (cumulative.shape[0], cumulative.shape[1])
    return outcome.reshape(count_of_heads, blocks * BLOCK, -1)

def finish(forward, backward, gate_flat, scale_row):
    summed = forward + backward
    normed = summed * lax.rsqrt(lax.optimization_barrier(jnp.mean(summed * summed, axis=-1, keepdims=True)) + EPSILON)
    flattened = normed.transpose(1, 0, 2).reshape(normed.shape[1], -1)
    return (jax.nn.sigmoid(gate_flat.astype(jnp.float32)) * flattened * scale_row).astype(jnp.bfloat16)

def direction(query_heads, key_heads, value_heads, write_rows, log_keep):
    count_of_heads, length, head_size = query_heads.shape
    blocks_in, summary = prepare(query_heads, key_heads, value_heads, write_rows, log_keep)
    start_state = (jnp.zeros((count_of_heads, head_size, head_size), jnp.float32), jnp.zeros((count_of_heads, head_size), jnp.float32), jnp.full((count_of_heads,), START_LEVEL, jnp.float32), jnp.zeros((count_of_heads,), jnp.float32))
    final_state, starts = block_starts(summary, start_state)
    return block_outputs(blocks_in, starts)

def group_output(query_flat, key_flat, value_flat, gate_flat, write_rows, keep_rows, scale_row, count_of_heads):
    query_heads = to_heads(query_flat, count_of_heads)
    key_heads = to_heads(key_flat, count_of_heads)
    value_heads = to_heads(value_flat, count_of_heads)
    log_keep = jax.nn.log_sigmoid(keep_rows)
    forward = direction(query_heads, key_heads, value_heads, write_rows[0], log_keep[0])
    backward = jnp.flip(direction(jnp.flip(query_heads, 1), jnp.flip(key_heads, 1), jnp.flip(value_heads, 1), jnp.flip(write_rows[1], -1), jnp.flip(log_keep[1], -1)), 1)
    return finish(forward, backward, gate_flat, scale_row)

def reference(residual, query_wide, key_wide, value_wide, gate_wide, write_wide, keep_wide, scale_wide, query_narrow, key_narrow, value_narrow, gate_narrow, write_narrow, keep_narrow, scale_narrow, output_wide, output_narrow, mixer_gain, up_weight, down_weight):
    wide_out = group_output(query_wide, key_wide, value_wide, gate_wide, write_wide, keep_wide, scale_wide, HW)
    narrow_out = group_output(query_narrow, key_narrow, value_narrow, gate_narrow, write_narrow, keep_narrow, scale_narrow, HN)
    mixed = jnp.dot(wide_out, output_wide, preferred_element_type=jnp.float32) + jnp.dot(narrow_out, output_narrow, preferred_element_type=jnp.float32)
    combined = residual.astype(jnp.float32) + mixed
    normed = (combined * lax.rsqrt(lax.optimization_barrier(jnp.mean(combined * combined, axis=-1, keepdims=True)) + EPSILON) * mixer_gain).astype(jnp.bfloat16)
    hidden = jnp.square(jax.nn.relu(jnp.dot(normed, up_weight, preferred_element_type=jnp.float32))).astype(jnp.bfloat16)
    return (combined + jnp.dot(hidden, down_weight, preferred_element_type=jnp.float32)).astype(jnp.bfloat16)
```

```python
import functools

import jax
import jax.numpy as jnp
from jax import lax
from jax.experimental import pallas as pl
from jax.experimental.pallas import tpu as pltpu
from jax.sharding import PartitionSpec as P

F32 = jnp.float32
BF16 = jnp.bfloat16
EPSILON = 1e-6
START = -1e30
LANES = 128
MESH = pl.DeviceIdType.MESH


def two_parts(x):
    high = x.astype(BF16)
    return high, (x - high.astype(F32)).astype(BF16)


def dot(a, b):
    return jnp.dot(a, b, preferred_element_type=F32)


def dot_nt(a, b):
    return lax.dot_general(a, b, (((1,), (1,)), ((), ())), preferred_element_type=F32)


def dot2(x, b):
    high, low = two_parts(x)
    return dot(high, b) + dot(low, b)


def stacked(rows):
    place = lax.broadcasted_iota(jnp.int32, (8, LANES), 0)
    result = jnp.zeros((8, LANES), F32)
    for k, row in enumerate(rows):
        result = jnp.where(place == k, jnp.broadcast_to(row, (8, LANES)), result)
    return result


def merged(early, late):
    top_w = jnp.maximum(late[3:4] + early[2:3], late[2:3])
    top_n = jnp.maximum(late[5:6] + early[4:5], late[4:5])
    fw = jnp.exp(late[3:4] + early[2:3] - top_w)
    lw = jnp.exp(late[2:3] - top_w)
    fn = jnp.exp(late[5:6] + early[4:5] - top_n)
    ln = jnp.exp(late[4:5] - top_n)
    rows = stacked(
        [
            fw * early[0:1] + lw * late[0:1],
            fn * early[1:2] + ln * late[1:2],
            top_w,
            early[3:4] + late[3:4],
            top_n,
            early[5:6] + late[5:6],
        ]
    )
    return fw, lw, fn, ln, rows


def layer(
    chips,
    ranks,
    res,
    qw,
    kw,
    vw,
    gw,
    write_w,
    keep_w,
    scale_w,
    qn,
    kn,
    vn,
    gn,
    write_n,
    keep_n,
    scale_n,
    ow,
    on,
    gain,
    up,
    down,
    out,
    wts,
    yall,
    wall,
    rall,
    mixed,
    normed,
    hidden,
    comb,
    lf8,
    wr8,
    b8,
    ct,
    va,
    nd,
    cc,
    fc,
    st,
    stp,
    tx1,
    rx1,
    tx2,
    rx2,
    runx,
    txj,
    rxj,
    cin,
    nm,
    pf,
    send_a,
    recv_a,
    send_b,
    recv_b,
    ring_s,
    ring_r,
    pair_s,
    pair_r,
    one_s,
    one_r,
    two_s,
    two_r,
    st_sem,
    x_s,
    x_r,
    w_s,
    w_r,
    a_s,
    a_r,
    b_s,
    b_r,
):
    tokens, width = qw.shape[0], res.shape[1]
    share = up.shape[0]
    block = res.shape[0]
    half_block = block // 2
    far = chips // 2
    piece = LANES // chips
    heads = write_n.shape[1]
    span = LANES // heads
    blocks = tokens // LANES

    grp = lax.axis_index("grp")
    s = lax.axis_index("sp")
    t = lax.axis_index("tp")
    z = s // 2
    c = s % 2
    step = 1 - 2 * c
    right = {"tp": lax.rem(t + 1, ranks)}
    left = {"tp": lax.rem(t + ranks - 1, ranks)}
    t_right = lax.rem(t + 1, ranks)
    t_left = lax.rem(t + ranks - 1, ranks)
    t_far = lax.rem(t + 2, ranks)
    partner = {"sp": 2 * z + 1 - c}
    onward = {"sp": 2 * lax.rem(z + step + chips, chips) + c}

    def chip(k):
        return lax.rem(z + k + chips, chips)

    def core_of(k):
        return {"sp": 2 * chip(k) + c}

    del grp
    barrier = pltpu.get_barrier_semaphore()
    met = [core_of(k) for k in range(1, chips)] + [partner, left, right]
    for device in met:
        pl.semaphore_signal(barrier, inc=1, device_id=device, device_id_type=MESH)

    sent = []

    def copy(src, dst, ss, rs, device):
        return pltpu.make_async_remote_copy(
            src_ref=src, dst_ref=dst, send_sem=ss, recv_sem=rs, device_id=device, device_id_type=MESH
        )

    def send(*args, when=None):
        op = copy(*args)
        op.start()
        if when is None:
            sent.append(op)
        return op

    own_row = pl.multiple_of(s * share, share)
    wts[0, pl.ds(own_row, share), :] = up[...]
    wts[1, pl.ds(own_row, share), :] = down[...]
    wall[t, 0] = ow[...]
    wall[t, 1] = on[...]
    rall[t] = res[...]

    lf8[...] = jnp.zeros_like(lf8)
    wr8[...] = jnp.zeros_like(wr8)
    for d in range(2):
        lf8[d * 3 : d * 3 + 1, :] = keep_w[d]
        lf8[d * 3 + 1 : d * 3 + 1 + heads, :] = keep_n[d]
        wr8[d * 3 : d * 3 + 1, :] = write_w[d]
        wr8[d * 3 + 1 : d * 3 + 1 + heads, :] = write_n[d]
    keep = lf8[...]
    log_keep = jnp.minimum(keep, 0.0) - jnp.log1p(jnp.exp(-jnp.abs(keep)))
    lane = lax.broadcasted_iota(jnp.int32, (8, tokens), 1)
    forward_row = lax.broadcasted_iota(jnp.int32, (8, tokens), 0) < 3

    def running(x, op, empty):
        shift = 1
        while shift < tokens:
            ahead = jnp.where(lane >= shift, pltpu.roll(x, shift, 1), empty)
            behind = jnp.where(lane < tokens - shift, pltpu.roll(x, tokens - shift, 1), empty)
            x = op(x, jnp.where(forward_row, ahead, behind))
            shift *= 2
        return x

    total8 = running(log_keep, jnp.add, 0.0)
    level8 = wr8[...] - total8
    peak8 = running(level8, jnp.maximum, -3e38)
    b8[...] = level8
    top8 = jnp.max(level8, axis=1, keepdims=True)
    sum8 = jnp.where(
        lax.broadcasted_iota(jnp.int32, (8, 1), 0) < 3, total8[:, tokens - 1 : tokens], total8[:, 0:1]
    )
    w8 = jnp.exp(level8 - top8)
    m8 = sum8 + top8
    ct[...] = jnp.transpose(jnp.concatenate([peak8, total8], axis=0))

    lane_row = lax.broadcasted_iota(jnp.int32, (1, LANES), 1)
    head_of_lane = lane_row // span
    sub = lax.broadcasted_iota(jnp.int32, (LANES, LANES), 0) // span
    lan = lax.broadcasted_iota(jnp.int32, (LANES, LANES), 1) // span
    same_head = sub == lan
    head_block = jnp.where(same_head, 1.0, 0.0).astype(BF16)
    all_ones = jnp.ones((LANES, LANES), BF16)
    head_sub = lax.broadcasted_iota(jnp.int32, (LANES, tokens), 0) // span

    def by_head(rows):
        result = jnp.broadcast_to(rows[0], (1, LANES))
        for h in range(1, heads):
            result = jnp.where(head_of_lane == h, jnp.broadcast_to(rows[h], (1, LANES)), result)
        return result

    ones_tail = jnp.ones((tokens, LANES), BF16)
    va[0, :, 0:LANES] = vw[...]
    va[0, :, LANES:] = ones_tail
    va[1, :, 0:LANES] = vn[...]
    va[1, :, LANES:] = ones_tail
    key_w = jnp.transpose(kw[...].astype(F32))
    key_n = jnp.transpose(kn[...].astype(F32))
    sums_w = dot2(w8, kw[...])
    sums_n = dot2(w8, kn[...])
    for d in range(2):
        r = d * 3
        cw = dot2(key_w * w8[r : r + 1], vw[...])
        weights = jnp.broadcast_to(w8[r + 1 : r + 2], (LANES, tokens))
        for h in range(1, heads):
            weights = jnp.where(head_sub == h, jnp.broadcast_to(w8[r + 1 + h : r + 2 + h], (LANES, tokens)), weights)
        cn = jnp.where(same_head, dot2(key_n * weights, vn[...]), 0.0)
        extra = stacked(
            [
                sums_w[r : r + 1],
                by_head([sums_n[r + 1 + h : r + 2 + h] for h in range(heads)]),
                jnp.broadcast_to(m8[r : r + 1], (1, LANES)),
                jnp.broadcast_to(sum8[r : r + 1], (1, LANES)),
                by_head([m8[r + 1 + h : r + 2 + h] for h in range(heads)]),
                by_head([sum8[r + 1 + h : r + 2 + h] for h in range(heads)]),
            ]
        )
        st[d, :, 0:piece, :] = cw.reshape(chips, piece, LANES)
        st[d, :, piece : 2 * piece, :] = cn.reshape(chips, piece, LANES)
        st[d, :, 2 * piece :, :] = jnp.broadcast_to(extra[None], (chips, 8, LANES))

    pl.semaphore_wait(barrier, len(met))

    def rows_at(k, o):
        core = c if o == 0 else 1 - c
        return pl.ds(pl.multiple_of((2 * chip(k) + core) * share, share), share)

    def ring_send(kind, j, o, src=None, when=None):
        rows = rows_at(-step * (j - 1), o)
        here = wts.at[kind, rows, :]
        return send(here if src is None else src, here, ring_s.at[kind, j, o], ring_r.at[kind, j, o], onward, when=when)

    def pair_send(kind, j, o, src=None, when=None):
        here = wts.at[kind, rows_at(-step * j, o), :]
        return send(here if src is None else src, here, pair_s.at[kind, j, o], pair_r.at[kind, j, o], partner, when=when)

    def ring_wait(kind, j, o):
        here = wts.at[kind, rows_at(-step * j, o), :]
        copy(here, here, ring_s.at[kind, j, o], ring_r.at[kind, j, o], onward).wait_recv()

    def pair_wait(kind, j, o):
        core = 1 - c if o == 0 else c
        rows = pl.ds(pl.multiple_of((2 * chip(step * j) + core) * share, share), share)
        here = wts.at[kind, rows, :]
        copy(here, here, pair_s.at[kind, j, o], pair_r.at[kind, j, o], partner).wait_recv()

    def ring_step(kind, j):
        for o in range(2):
            if j < far:
                ring_wait(kind, j, o)
                if j < far - 1:
                    ring_send(kind, j + 1, o)
                else:

                    @pl.when(c == kind)
                    def _():
                        ring_send(kind, j + 1, o, when=1)

                pair_send(kind, j, o)
            else:

                @pl.when(c == kind)
                def _():
                    ring_wait(kind, j, o)
                    pair_send(kind, j, o, when=1)

    def last_waits():
        for kind in range(2):

            @pl.when(c == kind)
            def _():
                for o in range(2):
                    rows = wts.at[kind, rows_at(-step * (far - 1), o), :]
                    copy(rows, rows, ring_s.at[kind, far, o], ring_r.at[kind, far, o], onward).wait_send()
                    rows = wts.at[kind, rows_at(-step * far, o), :]
                    copy(rows, rows, pair_s.at[kind, far, o], pair_r.at[kind, far, o], partner).wait_send()

    def pair_step(kind, j):
        for o in range(2):
            if j < far:
                pair_wait(kind, j, o)
            else:

                @pl.when(c != kind)
                def _():
                    pair_wait(kind, j, o)

    def x_start(kind, src, dst):
        send(src, dst, x_s.at[kind, 0], x_r.at[kind, 0], right)
        send(src, dst, x_s.at[kind, 1], x_r.at[kind, 1], left)

    def x_onward(kind, side, whole, part):
        device = right if side == 0 else left
        copy(whole, whole, x_s.at[kind, side], x_r.at[kind, side], left).wait_recv()
        send(part, part, x_s.at[kind, 2 + side], x_r.at[kind, 2 + side], device)

    def x_end(kind, side, part):
        copy(part, part, x_s.at[kind, 2 + side], x_r.at[kind, 2 + side], left).wait_recv()

    state_op = send(st.at[1 - c], stp, st_sem.at[0], st_sem.at[1], partner)
    for kind, own in ((0, up), (1, down)):
        pair_send(kind, 0, 0, src=own)
    ring_send(0, 1, 0, src=up)
    x_start(0, wall.at[t, c], wall.at[t, c])
    x_start(1, res, rall.at[t])

    state_op.wait_recv()
    mine = st[c, 0, 2 * piece :, :]
    fw, lw, fn, ln, extra = merged(mine, stp[0, 2 * piece :, :])
    for p in range(chips):
        tx1[p, 0:piece, :] = fw * st[c, p, 0:piece, :] + lw * stp[p, 0:piece, :]
        tx1[p, piece : 2 * piece, :] = fn * st[c, p, piece : 2 * piece, :] + ln * stp[p, piece : 2 * piece, :]
        tx1[p, 2 * piece :, :] = extra
    rx1[z] = tx1[z]
    order = sorted(range(1, chips), key=lambda k: -min(k, chips - k))
    for k in order:
        send(tx1.at[chip(k)], rx1.at[z], one_s.at[k], one_r.at[k], core_of(k))

    for kind in range(2):
        pair_wait(kind, 0, 0)
    ring_send(0, 1, 1)
    ring_send(1, 1, 0, src=down)
    ring_send(1, 1, 1)

    def inside(g, count, q_ref, k_ref, scale):
        def one(i, carry):
            r0 = pl.multiple_of(i * LANES, LANES)
            rows = pl.ds(r0, LANES)
            query = q_ref[rows, :]
            at = r0 + lax.broadcasted_iota(jnp.int32, (LANES, tokens), 0)
            of = lax.broadcasted_iota(jnp.int32, (LANES, tokens), 1)
            column = ct[rows, :]
            scores = []
            for h in range(count):
                part = query
                if count > 1:
                    part = query * jnp.where(head_of_lane == h, 1.0, 0.0).astype(BF16)
                scores.append(dot_nt(part, k_ref[...]) * scale)
            lane_head = lax.broadcasted_iota(jnp.int32, (LANES, 2 * LANES), 1) % LANES // span
            col_head = lax.broadcasted_iota(jnp.int32, (LANES, LANES), 1) // span
            for d in range(2):
                seen = of <= at if d == 0 else of >= at
                both = peak = total = None
                for h in range(count):
                    r = d * 3 + (0 if g == 0 else 1 + h)
                    c_col = column[:, r : r + 1]
                    f_col = column[:, 8 + r : 9 + r]
                    weight = jnp.exp(jnp.where(seen, b8[r : r + 1, :] - c_col, -1e30))
                    sums = dot2(weight * scores[h], va[g])
                    c_full = jnp.broadcast_to(c_col, (LANES, LANES))
                    f_full = jnp.broadcast_to(f_col, (LANES, LANES))
                    if h == 0:
                        both, peak, total = sums, c_full, f_full
                    else:
                        both = jnp.where(lane_head == h, sums, both)
                        peak = jnp.where(col_head == h, c_full, peak)
                        total = jnp.where(col_head == h, f_full, total)
                nd[g, d, rows, :] = both
                cc[g, d, rows, :] = peak
                fc[g, d, rows, :] = total
            return carry

        lax.fori_loop(0, blocks, one, 0)

    scales = (LANES**-0.5, span**-0.5)
    inside(0, 1, qw, kw, scales[0])
    ring_step(0, 1)
    inside(1, heads, qn, kn, scales[1])

    for k in range(1, chips):
        copy(rx1.at[z], rx1.at[chip(-k)], one_s.at[k], one_r.at[k], core_of(k)).wait_recv()

    def prefix(i, run):
        memory_w, memory_n, rows = run
        zi = i + c * (chips - 1 - 2 * i)
        tx2[zi, 0:piece, :] = memory_w
        tx2[zi, piece:, :] = memory_n
        runx[zi] = rows
        later = rx1[zi]
        fw, lw, fn, ln, new_rows = merged(rows, later[2 * piece :])
        return (
            fw * memory_w + lw * later[0:piece],
            fn * memory_n + ln * later[piece : 2 * piece],
            new_rows,
        )

    nothing = jnp.zeros((piece, LANES), F32)
    level = jnp.full((1, LANES), START, F32)
    zero_row = jnp.zeros((1, LANES), F32)
    lax.fori_loop(
        0,
        chips,
        prefix,
        (nothing, nothing, stacked([zero_row, zero_row, level, zero_row, level, zero_row])),
    )
    rx2[z] = tx2[z]
    for k in order:
        send(tx2.at[chip(k)], rx2.at[z], two_s.at[k], two_r.at[k], core_of(k))

    half = wall.shape[2] // 2

    def early_gathers():
        for side, slot, lo in ((0, t_left, 0), (1, t_right, half)):
            x_onward(0, side, wall.at[slot, c], wall.at[slot, c, pl.ds(lo, half), :])
            whole = wall.at[slot, c]
            send(whole, whole, w_s.at[side], w_r.at[side], partner)
        for side, slot, lo in ((0, t_left, 0), (1, t_right, half_block)):
            x_onward(1, side, rall.at[slot], rall.at[slot, pl.ds(lo, half_block), :])

    ring_step(0, 2) if far > 2 else None
    early_gathers()

    for k in range(1, chips):
        copy(rx2.at[z], rx2.at[chip(-k)], two_s.at[k], two_r.at[k], core_of(k)).wait_recv()
    incoming = runx[z]
    fw, lw, fn, ln, extra = merged(incoming, mine)
    for p in range(chips):
        txj[p, 0:piece, :] = fw * rx2[p, 0:piece, :] + lw * st[c, p, 0:piece, :]
        txj[p, piece : 2 * piece, :] = fn * rx2[p, piece : 2 * piece, :] + ln * st[c, p, piece : 2 * piece, :]
        txj[p, 2 * piece :, :] = extra
    nm[c] = incoming

    def put_memory(d, ref):
        for g in range(2):
            value = ref[:, g * piece : (g + 1) * piece, :].reshape(LANES, LANES)
            high, low = two_parts(value)
            cin[g, d, 0] = high
            cin[g, d, 1] = low

    put_memory(c, rx2)
    next_op = send(txj, rxj, st_sem.at[2], st_sem.at[3], partner)
    ring_step(0, 3) if far > 3 else None
    next_op.wait_recv()
    nm[1 - c] = rxj[0, 2 * piece :, :]
    put_memory(1 - c, rxj)

    def outcome(i, carry):
        rows = pl.ds(pl.multiple_of(i * LANES, LANES), LANES)
        for g, q_ref, gate, row in ((0, qw, gw, scale_w), (1, qn, gn, scale_n)):
            query = q_ref[rows, :]
            query_f = query.astype(F32)
            group = all_ones if g == 0 else head_block
            scale = scales[g]
            summed = None
            for d in range(2):
                carried = nm[d]
                level = carried[2 + 2 * g : 3 + 2 * g]
                peak = cc[g, d, rows, :]
                high = jnp.maximum(peak, level)
                inner = jnp.exp(peak - high)
                outer = jnp.exp(level - high) * scale
                floor = jnp.exp(-fc[g, d, rows, :] - high)
                far_sum = dot(query, cin[g, d, 0]) + dot(query, cin[g, d, 1])
                far_den = dot2(query_f * carried[g : g + 1], group)
                top = inner * nd[g, d, rows, 0:LANES] + outer * far_sum
                den = inner * nd[g, d, rows, LANES:] + outer * far_den
                part = top / jnp.maximum(jnp.abs(den), floor)
                summed = part if d == 0 else summed + part
            mean = dot2(summed * summed, group) * (1.0 / (LANES if g == 0 else span))
            gated = jax.nn.sigmoid(gate[rows, :].astype(F32)) * row[...]
            value = gated * (summed * lax.rsqrt(mean + EPSILON))
            yall[t, rows, g * LANES : (g + 1) * LANES] = value.astype(BF16)
        return carry

    lax.fori_loop(0, blocks, outcome, 0)
    ring_step(0, 4) if far > 4 else None
    x_start(2, yall.at[t], yall.at[t])

    tile = 2 * LANES

    def project(slot, first):
        def one(n, carry):
            cols = pl.ds(pl.multiple_of(n * tile, tile), tile)
            w = wall[slot, :, :, cols].reshape(tile, tile)
            part = dot(yall[slot], w)
            if first:
                mixed[:, cols] = part
            else:
                mixed[:, cols] += part
            return carry

        lax.fori_loop(0, width // tile, one, 0)

    for side, slot, lo in ((0, t_far, 0), (1, t_far, half)):
        part = wall.at[slot, c, pl.ds(lo, half), :]
        x_end(0, side, part)
        send(part, part, w_s.at[2 + side], w_r.at[2 + side], partner)
    project(t, True)
    other = 1 - c
    for side, slot in ((0, t_left), (1, t_right)):
        there = wall.at[slot, other]
        copy(there, there, w_s.at[side], w_r.at[side], partner).wait_recv()
    y_half = tokens // 2
    for side, slot, lo in ((0, t_left, 0), (1, t_right, y_half)):
        x_onward(2, side, yall.at[slot], yall.at[slot, pl.ds(lo, y_half), :])
    project(t_left, False)
    ring_step(0, 5) if far > 5 else None
    project(t_right, False)
    for side, lo in ((0, 0), (1, half)):
        there = wall.at[t_far, other, pl.ds(lo, half), :]
        copy(there, there, w_s.at[2 + side], w_r.at[2 + side], partner).wait_recv()
    for side, lo in ((0, 0), (1, half_block)):
        x_end(1, side, rall.at[t_far, pl.ds(lo, half_block), :])
    for side, lo in ((0, 0), (1, y_half)):
        x_end(2, side, yall.at[t_far, pl.ds(lo, y_half), :])
    project(t_far, False)
    ring_step(0, 6) if far > 6 else None

    chunk = 32

    def normalize(i, carry):
        rows = pl.ds(pl.multiple_of(i * chunk, chunk), chunk)
        slot = i // (block // chunk)
        inner = pl.ds(pl.multiple_of(lax.rem(i, block // chunk) * chunk, chunk), chunk)
        value = rall[slot, inner, :].astype(F32) + mixed[rows, :]
        mixed[rows, :] = value
        scale = lax.rsqrt(jnp.mean(value * value, axis=1, keepdims=True) + EPSILON)
        normed[rows, :] = (value * scale * gain[...]).astype(BF16)
        return carry

    lax.fori_loop(0, tokens // chunk, normalize, 0)
    comb[...] = mixed[pl.ds(pl.multiple_of(t * block, block), block), :]
    for j in range(7, far):
        ring_step(0, j)
    ring_step(0, far)
    for j in range(1, far + 1):
        pair_step(0, j)

    ring_step(1, 1)

    def raise_up(n, carry):
        cols = pl.ds(pl.multiple_of(n * tile, tile), tile)
        value = jnp.maximum(dot(normed[...], wts[0, :, cols]), 0.0)
        hidden[:, cols] = (value * value).astype(BF16)
        return carry

    lax.fori_loop(0, hidden.shape[1] // tile, raise_up, 0)

    def columns(k):
        first, second = (chip(k), chip(-k)) if k < far else (z, chip(far))
        return [pl.multiple_of(v * LANES, LANES) for v in (first, second)]

    def rows_of(rank, lo=0, count=None):
        return pl.ds(pl.multiple_of(rank * block + lo, half_block), block if count is None else count)

    def stage_mul(k):
        n = k - 1
        one, two = columns(k)
        w = jnp.concatenate([wts[1, pl.ds(one, LANES), :], wts[1, pl.ds(two, LANES), :]], axis=0)
        pf[n % 2] = dot_nt(hidden[...], w)
        send_a[n, 0] = pf[n % 2, rows_of(t_far, 0, half_block), :].astype(BF16)
        send_a[n, 1] = pf[n % 2, rows_of(t_far, half_block, half_block), :].astype(BF16)
        send(send_a.at[n, 0], recv_a.at[n, 0], a_s.at[n, 0], a_r.at[n, 0], right)
        send(send_a.at[n, 1], recv_a.at[n, 1], a_s.at[n, 1], a_r.at[n, 1], left)
        for i, at in enumerate((one, two)):
            comb[:, pl.ds(at, LANES)] += pf[n % 2, rows_of(t), i * LANES : (i + 1) * LANES]

    def stage_pass(k):
        n = k - 1
        for side in range(2):
            copy(send_a.at[n, side], recv_a.at[n, side], a_s.at[n, side], a_r.at[n, side], left).wait_recv()
        p = n % 2
        send_b[n, 0, 0:half_block] = (
            pf[p, rows_of(t_right, 0, half_block), :] + recv_a[n, 0].astype(F32)
        ).astype(BF16)
        send_b[n, 0, half_block:] = pf[p, rows_of(t_right, half_block, half_block), :].astype(BF16)
        send_b[n, 1, 0:half_block] = pf[p, rows_of(t_left, 0, half_block), :].astype(BF16)
        send_b[n, 1, half_block:] = (
            pf[p, rows_of(t_left, half_block, half_block), :] + recv_a[n, 1].astype(F32)
        ).astype(BF16)
        send(send_b.at[n, 0], recv_b.at[n, 0], b_s.at[n, 0], b_r.at[n, 0], right)
        send(send_b.at[n, 1], recv_b.at[n, 1], b_s.at[n, 1], b_r.at[n, 1], left)

    def stage_end(k):
        n = k - 1
        for side in range(2):
            copy(send_b.at[n, side], recv_b.at[n, side], b_s.at[n, side], b_r.at[n, side], left).wait_recv()
        for i, at in enumerate(columns(k)):
            here = slice(i * LANES, (i + 1) * LANES)
            value = comb[:, pl.ds(at, LANES)] + recv_b[n, 0, :, here].astype(F32) + recv_b[n, 1, :, here].astype(F32)
            out[:, pl.ds(at, LANES)] = value.astype(BF16)

    for k in range(1, far + 1):
        if k > 1:
            ring_step(1, k)
        pair_step(1, k)
        stage_mul(k)
        if k > 1:
            stage_pass(k - 1)
        if k > 2:
            stage_end(k - 2)
    stage_pass(far)
    if far > 1:
        stage_end(far - 1)
    stage_end(far)

    for op in sent:
        op.wait_send()
    last_waits()


def solution(mesh):
    chips, ranks = mesh.shape["sp"] // 2, mesh.shape["tp"]

    def body(*args):
        (res, qw, kw, vw, gw, ww, pw, sw, qn, kn, vn, gn, wn, pn, sn, ow, on, gain, up, down) = args
        tokens, width = qw.shape[0], res.shape[1]
        block, share, units = res.shape[0], up.shape[0], up.shape[1]
        piece, far = LANES // chips, chips // 2
        rows = 2 * piece + 8
        vm = pltpu.VMEM
        dma = pltpu.SemaphoreType.DMA
        scratch = [
            vm((2, width, units), BF16),
            vm((ranks, tokens, 2 * LANES), BF16),
            vm((ranks, 2, LANES, width), BF16),
            vm((ranks, block, width), BF16),
            vm((tokens, width), F32),
            vm((tokens, width), BF16),
            vm((tokens, units), BF16),
            vm((block, width), F32),
            vm((8, tokens), F32),
            vm((8, tokens), F32),
            vm((8, tokens), F32),
            vm((tokens, 16), F32),
            vm((2, tokens, 2 * LANES), BF16),
            vm((2, 2, tokens, 2 * LANES), F32),
            vm((2, 2, tokens, LANES), F32),
            vm((2, 2, tokens, LANES), F32),
            vm((2, chips, rows, LANES), F32),
            vm((chips, rows, LANES), F32),
            vm((chips, rows, LANES), F32),
            vm((chips, rows, LANES), F32),
            vm((chips, 2 * piece, LANES), F32),
            vm((chips, 2 * piece, LANES), F32),
            vm((chips, 8, LANES), F32),
            vm((chips, rows, LANES), F32),
            vm((chips, rows, LANES), F32),
            vm((2, 2, 2, LANES, LANES), BF16),
            vm((2, 8, LANES), F32),
            vm((2, tokens, 2 * LANES), F32),
            vm((far, 2, block // 2, 2 * LANES), BF16),
            vm((far, 2, block // 2, 2 * LANES), BF16),
            vm((far, 2, block, 2 * LANES), BF16),
            vm((far, 2, block, 2 * LANES), BF16),
            dma((2, far + 1, 2)),
            dma((2, far + 1, 2)),
            dma((2, far + 1, 2)),
            dma((2, far + 1, 2)),
            dma((chips,)),
            dma((chips,)),
            dma((chips,)),
            dma((chips,)),
            dma((4,)),
            dma((3, 4)),
            dma((3, 4)),
            dma((4,)),
            dma((4,)),
            dma((far, 2)),
            dma((far, 2)),
            dma((far, 2)),
            dma((far, 2)),
        ]
        return pl.pallas_call(
            functools.partial(layer, chips, ranks),
            out_shape=jax.ShapeDtypeStruct((block, width), BF16),
            in_specs=[pl.BlockSpec(memory_space=pltpu.VMEM)] * 20,
            out_specs=pl.BlockSpec(memory_space=pltpu.VMEM),
            scratch_shapes=scratch,
            compiler_params=pltpu.CompilerParams(
                collective_id=0, has_side_effects=True, vmem_limit_bytes=67043328
            ),
        )(
            res, qw, kw, vw, gw, ww, pw, sw.reshape(1, -1), qn, kn, vn, gn, wn, pn, sn.reshape(1, -1),
            ow, on, gain.reshape(1, -1), up, down.T,
        )

    places = (
        P(("grp", "sp", "tp"), None),
        *[P(("grp", "sp"), "tp")] * 4,
        *[P(None, "tp", ("grp", "sp"))] * 2,
        P("tp"),
        *[P(("grp", "sp"), "tp")] * 4,
        *[P(None, "tp", ("grp", "sp"))] * 2,
        P("tp"),
        P("tp", None),
        P("tp", None),
        P(),
        P("sp", "tp"),
        P("tp", "sp"),
    )
    return jax.shard_map(
        body, mesh=mesh, in_specs=places, out_specs=P(("grp", "sp", "tp"), None), check_vma=False
    )
```
